256 devices in a mesh: grp: 2 (over y), kv: 16 (over z), tp: 8 (over x, core).
Axes of the slice: x: 4, y: 2, z: 16, core: 2. Of those that a mesh axis runs over, the one named last changes fastest.
The devices are a block of a 4x16x16 slice.
Arguments:
- tokens: bfloat16 [16, 4096], P('grp', ('kv', 'tp')), parts along dimension 0, may hold values from -16 to 16
- key_cache: bfloat16 [16, 8192, 8, 256], P('grp', 'kv', 'tp'), parts along dimension 0, may hold values from -1200 to 1200
- value_cache: bfloat16 [16, 8192, 8, 256], P('grp', 'kv', 'tp'), parts along dimension 0, may hold values from -6 to 6
- gain_first: float32 [4096], replicated, may hold values from 0.1 to 1.9
- gate_first: bfloat16 [4096, 11008], P(None, ('kv', 'tp')), may hold values from -0.09375 to 0.09375
- up_first: bfloat16 [4096, 11008], P(None, ('kv', 'tp')), may hold values from -0.09375 to 0.09375
- down_first: bfloat16 [11008, 4096], P(('kv', 'tp')), may hold values from -0.0546875 to 0.0546875
- gain_mix: float32 [4096], replicated, may hold values from 0.1 to 1.9
- query_first: bfloat16 [4096, 1024], P('kv', 'tp'), may hold values from -0.09375 to 0.09375
- query_second: bfloat16 [4096, 1024], P('kv', 'tp'), may hold values from -0.09375 to 0.09375
- key_first: bfloat16 [4096, 1024], P('kv', 'tp'), may hold values from -0.5 to 0.5
- key_second: bfloat16 [4096, 1024], P('kv', 'tp'), may hold values from -0.5 to 0.5
- value_weight: bfloat16 [4096, 2048], P('kv', 'tp'), may hold values from -0.09375 to 0.09375
- mix_lambda: float32 [8], P('tp'), may hold values from 0.3 to 0.8
- head_gain: float32 [8, 256], P('tp'), may hold values from 0.1 to 1.9
- out_weight: bfloat16 [2048, 4096], P('tp', 'kv'), may hold values from -0.125 to 0.125
- gain_last: float32 [4096], replicated, may hold values from 0.1 to 1.9
- gate_last: bfloat16 [4096, 11008], P(None, ('kv', 'tp')), may hold values from -0.09375 to 0.09375
- up_last: bfloat16 [4096, 11008], P(None, ('kv', 'tp')), may hold values from -0.09375 to 0.09375
- down_last: bfloat16 [11008, 4096], P(('kv', 'tp')), may hold values from -0.0546875 to 0.0546875
Outputs:
- updated: bfloat16 [16, 4096], P('grp', ('kv', 'tp')), parts along dimension 0
The draws below stay inside these ranges and needn't reach their ends.
There are 2 independent parts, one for each index of `grp`. The reference program is written for one: setup_inputs(seed, part) draws one part's arguments, and reference() takes and returns one part's arrays. A program takes and returns all parts, laid end to end along the dimension named above; an argument that names none is the same for every part. Nothing has to cross between parts.
All inputs are finite; a program needn't handle non-finite values.
Results may differ from the reference program's by a relative error of at most 0.02.
Values may be sent and summed in bfloat16 or wider, within the bound.
A program may use at most 64 MiB of HBM per device.

```python
import jax
import jax.numpy as jnp
from jax import lax

D = 4096
FF = 11008
HEADS = 8
HEAD_DIM = 128
BATCH = 8
CTX_DEV = 512
CTX = 8192
N_KV = 16
N_TP = 8


def draw_tokens(key, part):
    normal_key = jax.random.fold_in(key, 11)
    column = jnp.arange(D)
    block_index = column // (D // (N_KV * N_TP))
    kv_place = (block_index // N_TP).astype(jnp.float32) / (N_KV - 1)
    tp_place = (block_index % N_TP).astype(jnp.float32) / (N_TP - 1)
    column_scale = 0.4 * 3.0 ** kv_place * 3.0 ** tp_place
    values = jax.random.normal(normal_key, (BATCH, D), jnp.float32) * column_scale
    return jnp.clip(values, -16.0, 16.0).astype(jnp.bfloat16)


def draw_key_cache(key, part):
    base_key = jax.random.fold_in(key, 21)
    shape = (BATCH, CTX, HEADS, 2 * HEAD_DIM)
    values = 1.75 * jax.random.normal(base_key, shape, jnp.float32)
    return jnp.clip(values, -1200.0, 1200.0).astype(jnp.bfloat16)


def shard_levels(stream_key, shape, shards, smallest, largest):
    gain, own = 1.0, jax.random.fold_in(stream_key, 6)
    for dim, blocks in shards:
        heights = jnp.exp(jax.random.uniform(jax.random.fold_in(own, dim), (blocks,), jnp.float32, smallest / len(shards), largest / len(shards)))
        gain = gain * jnp.repeat(heights, shape[dim] // blocks).reshape([-1 if axis == dim else 1 for axis in range(len(shape))])
    return gain


def scatter_about(stream_key, dims, spread, bound, shards=(), held_as=jnp.bfloat16):
    array = spread * jax.random.normal(stream_key, dims, jnp.float32)
    if shards:
        array = array * shard_levels(stream_key, dims, shards, -0.22, 0.18)
    return jnp.clip(array, -bound, bound).astype(held_as)


def setup_inputs(seed: int = 0, part: int = 0) -> dict:
    streams_of = jax.random.split(jax.random.key(seed), 21)
    own_keys = jax.random.split(jax.random.fold_in(streams_of[20], part), 21)
    return {
        "tokens": draw_tokens(jax.random.fold_in(jax.random.fold_in(streams_of[20], part), 71), part),
        "key_cache": draw_key_cache(jax.random.fold_in(jax.random.fold_in(streams_of[20], part), 71), part),
        "value_cache": scatter_about(own_keys[2], (BATCH, CTX, HEADS, 2 * HEAD_DIM), 1.0, 6.0, ((1, 16), (2, 8))),
        "gain_first": jnp.clip(1.0 + 0.18 * jax.random.normal(streams_of[3], (D,), jnp.float32), 0.1, 1.9),
        "gate_first": scatter_about(streams_of[4], (D, FF), D ** -0.5, 0.09375, ((1, 128),)),
        "up_first": scatter_about(streams_of[5], (D, FF), D ** -0.5, 0.09375, ((1, 128),)),
        "down_first": scatter_about(streams_of[6], (FF, D), FF ** -0.5, 0.0546875, ((0, 128),)),
        "gain_mix": jnp.clip(1.0 + 0.18 * jax.random.normal(streams_of[7], (D,), jnp.float32), 0.1, 1.9),
        "query_first": scatter_about(streams_of[8], (D, HEADS * HEAD_DIM), D ** -0.5, 0.09375, ((0, 16), (1, 8))),
        "query_second": scatter_about(streams_of[9], (D, HEADS * HEAD_DIM), D ** -0.5, 0.09375, ((0, 16), (1, 8))),
        "key_first": scatter_about(streams_of[10], (D, HEADS * HEAD_DIM), (D // 36) ** -0.5, 0.5, ((0, 16), (1, 8))),
        "key_second": scatter_about(streams_of[11], (D, HEADS * HEAD_DIM), (D // 36) ** -0.5, 0.5, ((0, 16), (1, 8))),
        "value_weight": scatter_about(streams_of[12], (D, HEADS * 2 * HEAD_DIM), D ** -0.5, 0.09375, ((0, 16), (1, 8))),
        "mix_lambda": jnp.clip(0.3 + 0.5 * jax.random.uniform(streams_of[13], (HEADS,), jnp.float32) ** shard_levels(streams_of[13], (HEADS,), ((0, 8),), -0.2, 0.2), 0.3, 0.8),
        "head_gain": jnp.clip(1.0 + 0.18 * jax.random.normal(streams_of[14], (HEADS, 2 * HEAD_DIM), jnp.float32), 0.1, 1.9),
        "out_weight": scatter_about(streams_of[15], (HEADS * 2 * HEAD_DIM, D), (HEADS * 2 * HEAD_DIM) ** -0.5, 0.125, ((0, 8), (1, 16))),
        "gain_last": jnp.clip(1.0 + 0.18 * jax.random.normal(streams_of[16], (D,), jnp.float32), 0.1, 1.9),
        "gate_last": scatter_about(streams_of[17], (D, FF), D ** -0.5, 0.09375, ((1, 128),)),
        "up_last": scatter_about(streams_of[18], (D, FF), D ** -0.5, 0.09375, ((1, 128),)),
        "down_last": scatter_about(streams_of[19], (FF, D), FF ** -0.5, 0.0546875, ((0, 128),)),
    }


norm_eps = 1e-06

def settle(values):
    return lax.optimization_barrier(values.astype(jnp.bfloat16))

def half_mixer(stream, gain_vec, weight_gate, weight_up, weight_down):
    wide_rows = stream.astype(jnp.float32)
    row_factor = lax.rsqrt(lax.optimization_barrier(jnp.mean(wide_rows * wide_rows, axis=-1, keepdims=True)) + norm_eps)
    normed = (wide_rows * gain_vec).astype(jnp.bfloat16)
    gate_value = row_factor * jnp.dot(normed, weight_gate, preferred_element_type=jnp.float32)
    up_value = row_factor * jnp.dot(normed, weight_up, preferred_element_type=jnp.float32)
    hidden = (jax.nn.silu(gate_value) * up_value).astype(jnp.bfloat16)
    mixed = jnp.dot(hidden, weight_down, preferred_element_type=jnp.float32)
    return settle(wide_rows + 0.5 * mixed)

def map_blocks(queries, key_block, value_block):
    scores = jnp.einsum('hd,nphd->nhp', queries.astype(jnp.float32), key_block.astype(jnp.float32)) * HEAD_DIM ** (-0.5)
    top_score = lax.optimization_barrier(jnp.max(scores, axis=-1))
    weights = jnp.exp(scores - top_score[..., None])
    weight_sum = lax.optimization_barrier(jnp.sum(weights, axis=-1))
    rounded = settle(weights).astype(jnp.float32)
    weighted = jnp.einsum('nhp,nphd->nhd', rounded, value_block.astype(jnp.float32))
    return (top_score, weight_sum, weighted)

def finish(stats, own_score, own_value):
    top_score, weight_sum, weighted = stats
    top_new = jnp.maximum(lax.optimization_barrier(jnp.max(top_score, axis=0)), own_score)
    factor_old = jnp.exp(top_score - top_new)
    factor_own = jnp.exp(own_score - top_new)
    total_sum = lax.optimization_barrier(jnp.sum(factor_old * weight_sum, axis=0)) + factor_own
    accum_sum = lax.optimization_barrier(jnp.sum(factor_old[..., None] * weighted, axis=0)) + factor_own[:, None] * own_value.astype(jnp.float32)
    return accum_sum / total_sum[:, None]

def attend_sequence(inputs):
    query_one, query_two, key_one, key_two, new_value, key_rows, value_rows, lam_vec = inputs
    key_block = key_rows.reshape(N_KV, CTX_DEV, HEADS, 2 * HEAD_DIM)
    value_block = value_rows.reshape(N_KV, CTX_DEV, HEADS, 2 * HEAD_DIM)
    stats_one = map_blocks(query_one, key_block[..., :HEAD_DIM], value_block)
    stats_two = map_blocks(query_two, key_block[..., HEAD_DIM:], value_block)
    own_one = lax.optimization_barrier(jnp.sum(query_one.astype(jnp.float32) * key_one.astype(jnp.float32), axis=-1)) * HEAD_DIM ** (-0.5)
    own_two = lax.optimization_barrier(jnp.sum(query_two.astype(jnp.float32) * key_two.astype(jnp.float32), axis=-1)) * HEAD_DIM ** (-0.5)
    return finish(stats_one, own_one, new_value) - lam_vec[:, None] * finish(stats_two, own_two, new_value)

def reference(tokens, key_cache, value_cache, gain_first, gate_first, up_first, down_first, gain_mix, query_first, query_second, key_first, key_second, value_weight, mix_lambda, head_gain, out_weight, gain_last, gate_last, up_last, down_last):
    first = half_mixer(tokens, gain_first, gate_first, up_first, down_first)
    mix_rows = first.astype(jnp.float32)
    mix_factor = lax.rsqrt(lax.optimization_barrier(jnp.mean(mix_rows * mix_rows, axis=-1, keepdims=True)) + norm_eps)
    normed = (mix_rows * gain_mix).astype(jnp.bfloat16)
    projected = [settle(mix_factor * jnp.dot(normed, weight, preferred_element_type=jnp.float32)) for weight in (query_first, query_second, key_first, key_second, value_weight)]
    query_one = projected[0].reshape(BATCH, HEADS, HEAD_DIM)
    query_two = projected[1].reshape(BATCH, HEADS, HEAD_DIM)
    key_one = projected[2].reshape(BATCH, HEADS, HEAD_DIM)
    key_two = projected[3].reshape(BATCH, HEADS, HEAD_DIM)
    new_value = projected[4].reshape(BATCH, HEADS, 2 * HEAD_DIM)
    lam_rows = jnp.broadcast_to(mix_lambda[None, :], (BATCH, HEADS))
    attended = lax.map(attend_sequence, (query_one, query_two, key_one, key_two, new_value, key_cache, value_cache, lam_rows))
    head_factor = lax.rsqrt(lax.optimization_barrier(jnp.mean(attended * attended, axis=-1, keepdims=True)) + norm_eps)
    headed = (attended * head_factor * head_gain).astype(jnp.bfloat16).reshape(BATCH, N_TP, HEADS // N_TP * 2 * HEAD_DIM)
    grouped_weight = out_weight.reshape(N_TP, HEADS // N_TP * 2 * HEAD_DIM, D)
    group_parts = settle(jnp.einsum('bgk,gkd->gbd', headed.astype(jnp.float32), grouped_weight.astype(jnp.float32)))
    projection = settle(lax.optimization_barrier(jnp.sum(group_parts.astype(jnp.float32), axis=0)))
    second = settle(first.astype(jnp.float32) + projection.astype(jnp.float32))
    return half_mixer(second, gain_last, gate_last, up_last, down_last)
```

```python
import functools

import jax
import jax.numpy as jnp
from jax import lax
from jax.experimental import pallas as pl
from jax.experimental.pallas import tpu as pltpu
from jax.sharding import PartitionSpec as P

MESH = pl.DeviceIdType.MESH
F32 = jnp.float32
BF16 = jnp.bfloat16
norm_eps = 1e-06
LOW = -1e30
LANES = 128

PHASES = 13
(A_TP, A_KV, B_TP, B_KV, D_Q, D_ROW, D_SQ, E_ACC, E_STAT, F_TP, G_KV, H_TP, H_KV) = range(PHASES)


def nt(a, b):
    return lax.dot_general(a, b, (((1,), (1,)), ((), ())), preferred_element_type=F32)


def nn(a, b):
    return lax.dot_general(a, b, (((1,), (0,)), ((), ())), preferred_element_type=F32)


def outward(n):
    return sorted(range(1, n), key=lambda k: (-min(k, n - k), k))


def layer_kernel(
    n_kv,
    n_tp,
    tokens,
    key_cache,
    value_cache,
    gain_first,
    gate_first,
    up_first,
    down_first,
    gain_mix,
    query_first,
    query_second,
    key_first,
    key_second,
    value_weight,
    mix_lambda,
    head_gain,
    out_weight,
    gain_last,
    gate_last,
    up_last,
    down_last,
    out_ref,
    tok_v,
    key_v,
    value_v,
    gains_v,
    gate_v,
    up_v,
    down_v,
    proj_v,
    lam_v,
    head_gain_v,
    out_v,
    a_tp,
    a_kv,
    g_kv,
    b_out,
    b_in,
    b_tp,
    h_out,
    h_in,
    h_half,
    h_tp,
    d_q,
    d_rows32,
    d_rows,
    d_rowr,
    d_sq,
    e_acc,
    e_stat,
    f_tp,
    load_sem,
    send_sem,
    recv_sem,
):
    kv = lax.axis_index("kv")
    tp = lax.axis_index("tp")
    rows, own = tokens.shape
    per_tile = LANES // own
    plane = own * n_tp
    width = plane * n_kv
    head_dim = query_first.shape[1]
    sizes = {"kv": n_kv, "tp": n_tp}
    here = {"kv": kv, "tp": tp}

    barrier = pltpu.get_barrier_semaphore()
    for axis in ("kv", "tp"):
        for k in range(1, sizes[axis]):
            peer = lax.rem(here[axis] + k, sizes[axis])
            pl.semaphore_signal(barrier, inc=1, device_id={axis: peer}, device_id_type=MESH)

    loads = []

    def load(src, dst):
        copy = pltpu.make_async_copy(src, dst, load_sem.at[len(loads)])
        copy.start()
        loads.append(copy)
        return copy

    load_tok = load(tokens, tok_v)
    load_first = [
        load(gain_first, gains_v.at[0]),
        load(gate_first, gate_v.at[0]),
        load(up_first, up_v.at[0]),
        load(down_first, down_v.at[0]),
    ]
    load_proj = [load(gain_mix, gains_v.at[1])]
    at = 0
    for weight in (query_first, query_second, key_first, key_second, value_weight):
        load_proj.append(load(weight, proj_v.at[:, pl.ds(at, weight.shape[1])]))
        at += weight.shape[1]
    load_cache = [load(key_cache, key_v), load(value_cache, value_v)]
    load_out = [load(mix_lambda, lam_v), load(head_gain, head_gain_v), load(out_weight, out_v)]
    load_last = [
        load(gain_last, gains_v.at[2]),
        load(gate_last, gate_v.at[1]),
        load(up_last, up_v.at[1]),
        load(down_last, down_v.at[1]),
    ]

    pl.semaphore_wait(barrier, n_kv + n_tp - 2)

    sends = []

    def send(axis, phase, k, src, dst):
        copy = pltpu.make_async_remote_copy(
            src_ref=src,
            dst_ref=dst.at[here[axis]],
            send_sem=send_sem.at[phase, k],
            recv_sem=recv_sem.at[phase, k],
            device_id={axis: lax.rem(here[axis] + k, sizes[axis])},
            device_id_type=MESH,
        )
        copy.start()
        sends.append(copy)

    def send_all(axis, phase, src_of, dst):
        for k in outward(sizes[axis]):
            send(axis, phase, k, src_of(lax.rem(here[axis] + k, sizes[axis])), dst)

    def arrived(axis, phase, dst, k):
        peer = lax.rem(here[axis] - k + sizes[axis], sizes[axis])
        pltpu.make_async_remote_copy(
            src_ref=dst.at[peer],
            dst_ref=dst.at[peer],
            send_sem=send_sem.at[phase, k],
            recv_sem=recv_sem.at[phase, k],
            device_id={axis: peer},
            device_id_type=MESH,
        ).wait_recv()
        return peer

    def all_arrived(axis, phase, dst):
        for k in reversed(outward(sizes[axis])):
            arrived(axis, phase, dst, k)

    lane = lax.broadcasted_iota(jnp.int32, (rows, LANES), 1)
    tile_place = lax.rem(tp, per_tile)
    tile_half = tp // per_tile

    def tp_gather(tile, phase, buf):
        buf[tp] = tile.astype(BF16)
        send_all("tp", phase, lambda peer: buf.at[tp], buf)
        all_arrived("tp", phase, buf)
        halves = []
        for first in range(0, n_tp, per_tile):
            total = buf[first].astype(F32)
            for t in range(first + 1, first + per_tile):
                total += buf[t].astype(F32)
            halves.append(total)
        return jnp.concatenate(halves, axis=1)

    def block_hidden(buf, phase, which):
        gate = jnp.zeros((rows, gate_v.shape[1]), F32)
        up = jnp.zeros((rows, up_v.shape[1]), F32)
        square = jnp.zeros((rows, 1), F32)
        for k in [0] + outward(n_kv)[::-1]:
            peer = kv if k == 0 else arrived("kv", phase, buf, k)
            columns = pl.ds(pl.multiple_of(peer * plane, plane), plane)
            wide = buf[peer].astype(F32)
            square += jnp.sum(wide * wide, axis=1, keepdims=True)
            normed = (wide * gains_v[which, :, columns]).astype(BF16)
            slot = 0 if which == 0 else 1
            gate += nt(normed, gate_v[slot, :, columns])
            up += nt(normed, up_v[slot, :, columns])
        factor = lax.rsqrt(square / width + norm_eps)
        gate, up = factor * gate, factor * up
        return (gate / (1.0 + jnp.exp(-gate)) * up).astype(BF16)

    def sum_over_kv(hidden, slot, phase, out_buf, in_buf):
        for k in outward(n_kv) + [0]:
            peer = lax.rem(kv + k, n_kv)
            columns = pl.ds(pl.multiple_of(peer * plane, plane), plane)
            part = nn(hidden, down_v[slot, :, columns]).astype(BF16)
            if k == 0:
                in_buf[kv] = part
            else:
                out_buf[k] = part
                send("kv", phase, k, out_buf.at[k], in_buf)
        all_arrived("kv", phase, in_buf)
        total = in_buf[0].astype(F32)
        for p in range(1, n_kv):
            total += in_buf[p].astype(F32)
        return total

    def sum_over_tp(phase, buf):
        all_arrived("tp", phase, buf)
        total = buf[0].astype(F32)
        for t in range(1, n_tp):
            total += buf[t].astype(F32)
        return total

    def wait(copies):
        for copy in copies:
            copy.wait()

    load_tok.wait()
    pick = lax.broadcasted_iota(jnp.int32, (own, LANES), 1) == (
        lax.broadcasted_iota(jnp.int32, (own, LANES), 0) + tile_place * own
    )
    tok_tile = nn(tok_v[...], pick.astype(F32).astype(BF16))
    tok_plane = tp_gather(tok_tile, A_TP, a_tp)
    a_kv[kv] = tok_plane.astype(BF16)
    send_all("kv", A_KV, lambda peer: a_kv.at[kv], a_kv)
    wait(load_first)
    hidden = block_hidden(a_kv, A_KV, 0)

    b_tp[tp] = sum_over_kv(hidden, 0, B_KV, b_out, b_in).astype(BF16)
    send_all("tp", B_TP, lambda peer: b_tp.at[tp], b_tp)
    first = (tok_plane + 0.5 * sum_over_tp(B_TP, b_tp)).astype(BF16).astype(F32)

    wait(load_proj)
    my_columns = pl.ds(pl.multiple_of(kv * plane, plane), plane)
    normed = (first * gains_v[1, :, my_columns]).astype(BF16)
    pair = 2 * head_dim
    d_q[kv] = nn(normed, proj_v[:, 0:pair]).astype(BF16)
    send_all("kv", D_Q, lambda peer: d_q.at[kv], d_q)
    square = jnp.sum(first * first, axis=1, keepdims=True)
    row_of = lax.broadcasted_iota(jnp.int32, (rows, LANES), 0)
    d_sq[kv] = jnp.sum(jnp.where(lane == row_of, square, 0.0), axis=0, keepdims=True)
    send_all("kv", D_SQ, lambda peer: d_sq.at[kv], d_sq)
    others = nn(normed, proj_v[:, pair:])
    groups = others.shape[1] // LANES
    for g in range(groups):
        d_rows32[pl.ds(g, rows, stride=groups), :] = others[:, g * LANES : (g + 1) * LANES]
    for b in range(rows):
        d_rows[b] = d_rows32[b * groups : (b + 1) * groups, :].astype(BF16)
    homes = n_kv // rows
    send_all("kv", D_ROW, lambda peer: d_rows.at[peer // homes], d_rowr)
    d_rowr[kv] = d_rows[kv // homes]

    all_arrived("kv", D_SQ, d_sq)
    square_row = d_sq[0]
    for p in range(1, n_kv):
        square_row += d_sq[p]
    square = jnp.sum(
        jnp.where(lane == row_of, jnp.broadcast_to(square_row, (rows, LANES)), 0.0), axis=1, keepdims=True
    )
    factor = lax.rsqrt(square / width + norm_eps)
    all_arrived("kv", D_Q, d_q)
    query = d_q[0].astype(F32)
    for p in range(1, n_kv):
        query += d_q[p].astype(F32)
    query = (factor * query).astype(BF16).astype(F32)

    wait(load_cache)
    both = 2 * rows
    scale = head_dim ** (-0.5)
    zero = jnp.zeros((rows, head_dim), F32)
    stacked = jnp.concatenate(
        [
            jnp.concatenate([query[:, :head_dim], zero], axis=1),
            jnp.concatenate([zero, query[:, head_dim:]], axis=1),
        ],
        axis=0,
    )
    sequence = lax.rem(lax.broadcasted_iota(jnp.int32, (both, 1), 0), rows)
    scores = None
    for b in range(rows):
        term = nt(jnp.where(sequence == b, stacked, 0.0).astype(BF16), key_v[b])
        scores = term if scores is None else scores + term
    scores = scores * scale
    top = jnp.max(scores, axis=1, keepdims=True)
    weights = jnp.exp(scores - top)
    weight_sum = jnp.sum(weights, axis=1, keepdims=True)
    weighted = None
    for b in range(rows):
        term = nn(jnp.where(sequence == b, weights, 0.0).astype(BF16), value_v[b])
        weighted = term if weighted is None else weighted + term

    all_arrived("kv", D_ROW, d_rowr)
    own_rows = d_rowr[0].astype(F32)
    for p in range(1, n_kv):
        own_rows += d_rowr[p].astype(F32)
    my_row = kv // homes
    is_mine = sequence == my_row
    own_factor = jnp.sum(
        jnp.where(lax.broadcasted_iota(jnp.int32, (rows, 1), 0) == my_row, factor, 0.0), axis=0, keepdims=True
    )
    own_rows = (own_factor * own_rows).astype(BF16).astype(F32)
    own_keys = jnp.concatenate([own_rows[0:1], own_rows[1:2]], axis=1)
    own_value = jnp.concatenate([own_rows[2:3], own_rows[3:4]], axis=1)
    own_score = jnp.sum(stacked * own_keys, axis=1, keepdims=True) * scale
    is_home = jnp.logical_and(is_mine, lax.rem(kv, homes) == 0)
    own_score = jnp.where(is_home, own_score, LOW)
    new_top = jnp.maximum(top, own_score)
    old_factor = jnp.exp(top - new_top)
    own_weight = jnp.where(is_home, jnp.exp(own_score - new_top), 0.0)
    weight_sum = old_factor * weight_sum + own_weight
    weighted = old_factor * weighted + own_weight * own_value
    top = new_top

    wide_lane = lax.broadcasted_iota(jnp.int32, (both, LANES), 1)
    wide_row = lax.broadcasted_iota(jnp.int32, (both, LANES), 0)
    diagonal = wide_lane == wide_row
    as_row = lambda column: jnp.sum(jnp.where(diagonal, column, 0.0), axis=0, keepdims=True)
    as_column = lambda row: jnp.sum(
        jnp.where(diagonal, jnp.broadcast_to(row, (both, LANES)), 0.0), axis=1, keepdims=True
    )
    e_acc[kv] = weighted.astype(BF16)
    e_stat[kv] = jnp.concatenate([as_row(top), as_row(weight_sum)], axis=0)
    send_all("kv", E_STAT, lambda peer: e_stat.at[kv], e_stat)
    send_all("kv", E_ACC, lambda peer: e_acc.at[kv], e_acc)
    all_arrived("kv", E_STAT, e_stat)
    stats = [e_stat[p] for p in range(n_kv)]
    top_row = functools.reduce(jnp.maximum, [s[0:1] for s in stats])
    shares = [jnp.exp(s[0:1] - top_row) for s in stats]
    total_row = functools.reduce(jnp.add, [f * s[1:2] for f, s in zip(shares, stats)])
    columns = [as_column(f) for f in shares]
    total = as_column(total_row)
    all_arrived("kv", E_ACC, e_acc)
    merged = functools.reduce(jnp.add, [c * e_acc[p].astype(F32) for p, c in enumerate(columns)])
    merged = merged / total
    wait(load_out)
    attended = merged[:rows] - lam_v[...] * merged[rows:]
    head_factor = lax.rsqrt(jnp.mean(attended * attended, axis=1, keepdims=True) + norm_eps)
    headed = (attended * head_factor * head_gain_v[...]).astype(BF16)

    f_tp[tp] = nn(headed, out_v[...]).astype(BF16)
    send_all("tp", F_TP, lambda peer: f_tp.at[tp], f_tp)
    projection = sum_over_tp(F_TP, f_tp)
    second = (first + projection.astype(BF16).astype(F32)).astype(BF16)

    g_kv[kv] = second
    send_all("kv", G_KV, lambda peer: g_kv.at[kv], g_kv)
    wait(load_last)
    hidden = block_hidden(g_kv, G_KV, 2)
    summed = sum_over_kv(hidden, 1, H_KV, h_out, h_in).astype(BF16)
    second = second.astype(F32)
    second_tile = jnp.zeros((rows, LANES), F32)
    for half in range(n_tp // per_tile):
        tile = slice(half * LANES, (half + 1) * LANES)
        h_half[half] = summed[:, tile]
        second_tile = jnp.where(tile_half == half, second[:, tile], second_tile)
    send_all("tp", H_TP, lambda peer: h_half.at[peer // per_tile], h_tp)
    h_tp[tp] = h_half[tile_half]
    updated = second_tile + 0.5 * sum_over_tp(H_TP, h_tp)
    turn = lax.rem(per_tile - tile_place, per_tile) * own
    out_ref[...] = pltpu.roll(updated, turn, 1)[:, :own].astype(BF16)
    for copy in sends:
        copy.wait_send()


def solution(mesh):
    n_kv, n_tp = mesh.shape["kv"], mesh.shape["tp"]
    both_axes = ("kv", "tp")

    def step(*args):
        (
            tokens,
            key_cache,
            value_cache,
            gain_first,
            gate_first,
            up_first,
            down_first,
            gain_mix,
            query_first,
            query_second,
            key_first,
            key_second,
            value_weight,
            mix_lambda,
            head_gain,
            out_weight,
            gain_last,
            gate_last,
            up_last,
            down_last,
        ) = args
        rows, own = tokens.shape
        plane = own * n_tp
        width = plane * n_kv
        hidden = gate_first.shape[1]
        positions, head_width = key_cache.shape[1], key_cache.shape[3]
        proj_width = 2 * query_first.shape[1] + 2 * key_first.shape[1] + value_weight.shape[1]
        groups = (proj_width - 2 * query_first.shape[1]) // LANES
        cache_shape = (rows, positions, head_width)
        operands = (
            tokens,
            key_cache.reshape(cache_shape),
            value_cache.reshape(cache_shape),
            gain_first.reshape(1, width),
            gate_first.T,
            up_first.T,
            down_first,
            gain_mix.reshape(1, width),
            query_first,
            query_second,
            key_first,
            key_second,
            value_weight,
            mix_lambda.reshape(1, 1),
            head_gain,
            out_weight,
            gain_last.reshape(1, width),
            gate_last.T,
            up_last.T,
            down_last,
        )
        scratch = [
            pltpu.VMEM((rows, own), BF16),
            pltpu.VMEM(cache_shape, BF16),
            pltpu.VMEM(cache_shape, BF16),
            pltpu.VMEM((3, 1, width), F32),
            pltpu.VMEM((2, hidden, width), BF16),
            pltpu.VMEM((2, hidden, width), BF16),
            pltpu.VMEM((2, hidden, width), BF16),
            pltpu.VMEM((plane, proj_width), BF16),
            pltpu.VMEM((1, 1), F32),
            pltpu.VMEM((1, head_width), F32),
            pltpu.VMEM(out_weight.shape, BF16),
            pltpu.VMEM((n_tp, rows, LANES), BF16),
            pltpu.VMEM((n_kv, rows, plane), BF16),
            pltpu.VMEM((n_kv, rows, plane), BF16),
            pltpu.VMEM((n_kv, rows, plane), BF16),
            pltpu.VMEM((n_kv, rows, plane), BF16),
            pltpu.VMEM((n_tp, rows, plane), BF16),
            pltpu.VMEM((n_kv, rows, plane), BF16),
            pltpu.VMEM((n_kv, rows, plane), BF16),
            pltpu.VMEM((plane // LANES, rows, LANES), BF16),
            pltpu.VMEM((n_tp, rows, LANES), BF16),
            pltpu.VMEM((n_kv, rows, 2 * query_first.shape[1]), BF16),
            pltpu.VMEM((rows * groups, LANES), F32),
            pltpu.VMEM((rows, groups, LANES), BF16),
            pltpu.VMEM((n_kv, groups, LANES), BF16),
            pltpu.VMEM((n_kv, 1, LANES), F32),
            pltpu.VMEM((n_kv, 2 * rows, head_width), BF16),
            pltpu.VMEM((n_kv, 2, LANES), F32),
            pltpu.VMEM((n_tp, rows, plane), BF16),
            pltpu.SemaphoreType.DMA((len(operands),)),
            pltpu.SemaphoreType.DMA((PHASES, max(n_kv, n_tp))),
            pltpu.SemaphoreType.DMA((PHASES, max(n_kv, n_tp))),
        ]
        return pl.pallas_call(
            functools.partial(layer_kernel, n_kv, n_tp),
            out_shape=jax.ShapeDtypeStruct((rows, own), BF16),
            in_specs=[pl.BlockSpec(memory_space=pl.ANY)] * len(operands),
            out_specs=pl.BlockSpec(memory_space=pltpu.VMEM),
            scratch_shapes=scratch,
            compiler_params=pltpu.CompilerParams(collective_id=0, has_side_effects=True),
            name="layer",
        )(*operands)

    in_specs = (
        P("grp", both_axes),
        P("grp", "kv", "tp", None),
        P("grp", "kv", "tp", None),
        P(),
        P(None, both_axes),
        P(None, both_axes),
        P(both_axes, None),
        P(),
        P("kv", "tp"),
        P("kv", "tp"),
        P("kv", "tp"),
        P("kv", "tp"),
        P("kv", "tp"),
        P("tp"),
        P("tp", None),
        P("tp", "kv"),
        P(),
        P(None, both_axes),
        P(None, both_axes),
        P(both_axes, None),
    )
    return jax.shard_map(step, mesh=mesh, in_specs=in_specs, out_specs=P("grp", both_axes), check_vma=False)
```
